128 devices in a mesh: fs: 16 (over z, x), rep: 4 (over y), tp: 2 (over core).
Axes of the slice: x: 4, y: 4, z: 4, core: 2. Of those that a mesh axis runs over, the one named last changes fastest.
Arguments:
- saved_query: bfloat16 [196608, 512], P(('fs', 'rep')), may hold values from -30 to 30
- upstream_query: bfloat16 [196608, 1536], P(('fs', 'rep'), 'tp'), may hold values from -0.067658235 to 0.067658235
- weight_query: float32 [512, 1536], P('fs', 'tp'), may hold values from -0.25 to 0.25
- moment_query: float32 [512, 1536], P('fs', 'tp'), may hold values from -12 to 12
- left_query: bfloat16 [512, 512], P('fs'), may hold values from -2 to 2
- right_query: bfloat16 [4, 384, 384], P('tp'), may hold values from -2 to 2
- saved_output: bfloat16 [196608, 1024], P(('fs', 'rep')), may hold values from -30 to 30
- upstream_output: bfloat16 [196608, 2048], P(('fs', 'rep'), 'tp'), may hold values from -0.067658235 to 0.067658235
- weight_output: float32 [1024, 2048], P('fs', 'tp'), may hold values from -0.1875 to 0.1875
- moment_output: float32 [1024, 2048], P('fs', 'tp'), may hold values from -12 to 12
- left_output: bfloat16 [1024, 1024], P('fs'), may hold values from -2 to 2
- right_output: bfloat16 [4, 512, 512], P('tp'), may hold values from -2 to 2
Outputs:
- new_weight_query: float32 [512, 1536], P('fs', 'tp')
- new_moment_query: float32 [512, 1536], P('fs', 'tp')
- copy_query: bfloat16 [512, 1536], P(None, 'tp')
- new_weight_output: float32 [1024, 2048], P('fs', 'tp')
- new_moment_output: float32 [1024, 2048], P('fs', 'tp')
- copy_output: bfloat16 [1024, 2048], P(None, 'tp')
The draws below stay inside these ranges and needn't reach their ends.
All inputs are finite; a program needn't handle non-finite values.
Results may differ from the reference program's by a relative error of at most 0.0085.
Values may be sent and summed in bfloat16 or wider, within the bound.
A program may use at most 128 MiB of HBM per device.

```python
import jax
import jax.numpy as jnp
from jax import lax

QL = 512
QCOLS = 1536
VW = 1024
DM = 2048
QBLK = 384
OBLK = 512
TOKENS = 196608


def scaled_normal(key, rows, cols, unit):
    first, second = jax.random.split(key, 2)
    ramp = 3.0 ** (jnp.arange(cols, dtype=jnp.float32) / cols)
    rough = jnp.exp(jax.random.uniform(second, (cols,), jnp.float32, -0.5, 0.5))
    base = jnp.clip(jax.random.normal(first, (rows, cols), jnp.float32), -6.0, 6.0)
    return (base * ramp * rough * unit).astype(jnp.bfloat16)


def root_factor(key, count, size):
    first, second = jax.random.split(key)
    diag = jax.random.uniform(first, (count, size), jnp.float32, 0.6, 1.4)
    off = jnp.clip(jax.random.normal(second, (count, size, size), jnp.float32), -4.0, 4.0)
    off = off * (0.6 / size ** 0.5)
    off = 0.5 * (off + jnp.swapaxes(off, 1, 2))
    eye = jnp.eye(size, dtype=jnp.float32)
    return (off * (1.0 - eye) + diag[:, :, None] * eye).astype(jnp.bfloat16)


def draw_saved_query(key, part):
    return scaled_normal(jax.random.fold_in(key, 11), TOKENS, QL, 1.0)


def draw_upstream_query(key, part):
    return scaled_normal(jax.random.fold_in(key, 12), TOKENS, QCOLS, TOKENS ** (-0.5))


def draw_left_query(key, part):
    return root_factor(jax.random.fold_in(key, 13), 1, QL)[0]


def draw_right_query(key, part):
    return root_factor(jax.random.fold_in(key, 14), QCOLS // QBLK, QBLK)


def draw_saved_output(key, part):
    return scaled_normal(jax.random.fold_in(key, 21), TOKENS, VW, 1.0)


def draw_upstream_output(key, part):
    return scaled_normal(jax.random.fold_in(key, 22), TOKENS, DM, TOKENS ** (-0.5))


def draw_left_output(key, part):
    return root_factor(jax.random.fold_in(key, 23), 1, VW)[0]


def draw_right_output(key, part):
    return root_factor(jax.random.fold_in(key, 24), DM // OBLK, OBLK)


def level_of(key, shape, cuts, smallest, largest):
    level, own = 1.0, jax.random.fold_in(key, 6)
    for axis_at, shards_of in cuts:
        steps = jnp.exp(jax.random.uniform(jax.random.fold_in(own, axis_at), (shards_of,), jnp.float32, smallest / len(cuts), largest / len(cuts)))
        level = level * jnp.repeat(steps, shape[axis_at] // shards_of).reshape([-1 if axis == axis_at else 1 for axis in range(len(shape))])
    return level


def bell_draw(rng, extent, scale, bound, cuts=(), held_as=jnp.bfloat16):
    values = jax.random.normal(rng, extent, jnp.float32) * scale
    if len(cuts) > 0:
        values = level_of(rng, extent, cuts, -0.22, 0.18) * values
    return jnp.clip(values, min=-bound, max=bound).astype(held_as)


def setup_inputs(seed: int = 0) -> dict:
    splits = jax.random.split(jax.random.key(seed), 13)
    return {
        "saved_query": draw_saved_query(jax.random.fold_in(splits[12], 71), 0),
        "upstream_query": draw_upstream_query(jax.random.fold_in(splits[12], 71), 0),
        "weight_query": bell_draw(splits[2], (QL, QCOLS), QL ** -0.5, 0.25, ((0, 16), (1, 2)), jnp.float32),
        "moment_query": bell_draw(splits[3], (QL, QCOLS), 2.0, 12.0, ((0, 16), (1, 2)), jnp.float32),
        "left_query": draw_left_query(jax.random.fold_in(splits[12], 71), 0),
        "right_query": draw_right_query(jax.random.fold_in(splits[12], 71), 0),
        "saved_output": draw_saved_output(jax.random.fold_in(splits[12], 71), 0),
        "upstream_output": draw_upstream_output(jax.random.fold_in(splits[12], 71), 0),
        "weight_output": bell_draw(splits[8], (VW, DM), VW ** -0.5, 0.1875, ((0, 16), (1, 2)), jnp.float32),
        "moment_output": bell_draw(splits[9], (VW, DM), 2.0, 12.0, ((0, 16), (1, 2)), jnp.float32),
        "left_output": draw_left_output(jax.random.fold_in(splits[12], 71), 0),
        "right_output": draw_right_output(jax.random.fold_in(splits[12], 71), 0),
    }


def precondition(saved, upstream, left, right, block):
    grad = lax.dot_general(saved, upstream, (((0,), (0,)), ((), ())), preferred_element_type=jnp.float32)
    rounded = grad.astype(jnp.bfloat16)
    left_prod = jnp.dot(left, rounded, preferred_element_type=jnp.float32).astype(jnp.bfloat16)
    rows = left_prod.shape[0]
    shaped = left_prod.reshape(rows, -1, block).astype(jnp.float32)
    direction = jnp.einsum('rnb,nbc->rnc', shaped, right.astype(jnp.float32)).reshape(rows, -1)
    return (grad, direction)

def finish(weight, moment, direction, scale):
    new_moment = 0.8 * moment + scale * direction
    new_weight = 0.998 * weight - 0.02 * new_moment
    return (new_weight, new_moment, new_weight.astype(jnp.bfloat16))

def reference(saved_query, upstream_query, weight_query, moment_query, left_query, right_query, saved_output, upstream_output, weight_output, moment_output, left_output, right_output):
    grad_q, dir_q = precondition(saved_query, upstream_query, left_query, right_query, QBLK)
    grad_o, dir_o = precondition(saved_output, upstream_output, left_output, right_output, OBLK)
    scale_q = jnp.sqrt(jnp.sum(grad_q * grad_q) / (jnp.sum(dir_q * dir_q) + 1e-06))
    scale_o = jnp.sqrt(jnp.sum(grad_o * grad_o) / (jnp.sum(dir_o * dir_o) + 1e-06))
    wq, mq, cq = finish(weight_query, moment_query, dir_q, scale_q)
    wo, mo, co = finish(weight_output, moment_output, dir_o, scale_o)
    return (wq, mq, cq, wo, mo, co)
```

```python
import functools

import jax
import jax.numpy as jnp
from jax import lax
from jax.experimental import pallas as pl
from jax.experimental.pallas import tpu as pltpu
from jax.sharding import PartitionSpec as P

MESH = pl.DeviceIdType.MESH
BF = jnp.bfloat16
F32 = jnp.float32
HBM = pl.BlockSpec(memory_space=pl.ANY)

TOK = 3072
STREAMS = {"q": (16, 16, 16), "a": (16, 32, 16), "b": (16, 16, 32)}
ORDER = ("xyz", "yzx", "zxy")


def vmem_scratch():
    s = {}
    s["uq"] = ((TOK, 768), BF)
    s["sq"] = ((TOK, 512), BF)
    s["uo"] = ((TOK, 1024), BF)
    s["so"] = ((TOK, 1024), BF)
    s["rq"] = ((2, 384, 384), BF)
    s["ro"] = ((2, 512, 512), BF)
    s["wq"] = ((32, 768), F32)
    s["mq"] = ((32, 768), F32)
    s["wo"] = ((64, 1024), F32)
    s["mo"] = ((64, 1024), F32)
    s["lq"] = ((4, 32, 512), BF)
    s["lo"] = ((4, 64, 1024), BF)
    for c, rows in STREAMS.items():
        for t, nr in enumerate(rows):
            s[f"a1{c}{t}"] = ((4, 16 * nr, 128), BF)
            s[f"r1{c}{t}"] = ((3, 16 * nr, 128), BF)
            s[f"a2{c}{t}"] = ((4, 4 * nr, 128), BF)
            s[f"r2{c}{t}"] = ((3, 4 * nr, 128), BF)
            s[f"a3{c}{t}"] = ((4, nr, 128), BF)
            s[f"r3{c}{t}"] = ((3, nr, 128), BF)
    s["gq"] = ((4, 48, 128), BF)
    s["go"] = ((2, 4, 64, 128), BF)
    s["psq"] = ((64, 128), BF)
    s["pq"] = ((16, 64, 128), BF)
    s["pso"] = ((4, 48, 128), BF)
    s["po"] = ((16, 48, 128), BF)
    s["dq"] = ((128, 768), F32)
    s["do"] = ((64, 1024), F32)
    for c in "qo":
        s[f"cs{c}"] = ((16, 128), F32)
        s[f"cr{c}"] = ((16, 128), F32)
        s[f"ps{c}2"] = ((8, 128), F32)
        s[f"pr{c}2"] = ((16, 8, 128), F32)
    s["cq"] = ((4, 4, 32, 768), BF)
    s["co"] = ((4, 4, 64, 1024), BF)
    return s


SCRATCH = vmem_scratch()


class Sems:
    def __init__(self, ref):
        self.ref = ref
        self.n = 0

    def new(self):
        self.n += 1
        return self.ref.at[self.n - 1]


N_SEMS = 200


def kernel(*refs):
    names = [
        f"{n}_{k}" for k in "qo" for n in ("saved", "up", "weight", "moment", "left", "right")
    ]
    i = dict(zip(names, refs[:12]))
    o_wq, o_mq, o_cq, o_wo, o_mo, o_co = refs[12:18]
    v = dict(zip(SCRATCH, refs[18 : 18 + len(SCRATCH)]))
    sems = Sems(refs[18 + len(SCRATCH)])

    fs = lax.axis_index("fs")
    y = lax.axis_index("rep")
    c = lax.axis_index("tp")
    z = lax.div(fs, 4)
    x = lax.rem(fs, 4)
    me = {"x": x, "y": y, "z": z}

    def off(d, k):
        return lax.rem(me[d] + k, 4)

    def dev(dz=0, dx=0, dy=0, dc=0):
        return (
            lax.rem(z + dz, 4) * 4 + lax.rem(x + dx, 4),
            lax.rem(y + dy, 4),
            lax.rem(c + dc, 2),
        )

    def along(d, k):
        return dev(**{"d" + d: k})

    sent = []

    def local(src, dst):
        sem = sems.new()
        cp = pltpu.make_async_copy(src, dst, sem)
        cp.start()
        return cp

    def send(src, dst, ss, rs, to):
        pltpu.make_async_remote_copy(
            src_ref=src, dst_ref=dst, send_sem=ss, recv_sem=rs, device_id=to, device_id_type=MESH
        ).start()

    def wait(ref, sem):
        pltpu.make_async_copy(ref, ref, sem).wait()

    ld = {}
    ld["uq"] = local(i["up_q"], v["uq"])
    ld["sq"] = local(i["saved_q"], v["sq"])
    ld["lo"] = local(i["left_o"], v["lo"].at[x])
    ld["lq"] = local(i["left_q"], v["lq"].at[x])
    for h in range(2):
        for k in range(4):
            ld[f"so{h}{k}"] = local(
                i["saved_o"].at[:, pl.ds((k * 2 + h) * 128, 128)],
                v["so"].at[:, pl.ds((h * 4 + k) * 128, 128)],
            )
        if h == 0:
            ld["uo"] = local(i["up_o"], v["uo"])
    ld["rq"] = local(i["right_q"], v["rq"])
    ld["ro"] = local(i["right_o"], v["ro"])
    for n, k in (("weight_q", "wq"), ("moment_q", "mq"), ("weight_o", "wo"), ("moment_o", "mo")):
        ld[k] = local(i[n], v[k])

    peers = [dict(dc=1)]
    peers += [dict(dx=a, dy=b) for a in range(4) for b in range(4) if a or b]
    peers += [dict(dz=a, dx=b) for a in range(1, 4) for b in range(4)]
    barrier = pltpu.get_barrier_semaphore()
    for p in peers:
        pl.semaphore_signal(barrier, inc=1, device_id=dev(**p), device_id_type=MESH)
    pl.semaphore_wait(barrier, len(peers))

    def left_start(k, half):
        ld[k].wait()
        ss, rs = sems.new(), sems.new()
        part = v[k].at[x, pl.ds(c * half, half)]
        for d in (1, 2, 3):
            send(part, part, ss, rs, along("x", d))
        sent.append((v[k].at[pl.ds(0, 3), pl.ds(0, half)], ss))
        return rs

    lsem = {"lo": left_start("lo", 32), "lq": left_start("lq", 16)}

    def left_forward(k, half):
        wait(v[k].at[pl.ds(0, 3), pl.ds(0, half)], lsem[k])
        ss, rs = sems.new(), sems.new()
        for d in (1, 2, 3):
            part = v[k].at[off("x", d), pl.ds(c * half, half)]
            send(part, part, ss, rs, dev(dc=1))
        sent.append((v[k].at[pl.ds(0, 3), pl.ds(0, half)], ss))
        lsem[k] = rs

    def left_done(k, half):
        wait(v[k].at[pl.ds(0, 3), pl.ds(0, half)], lsem[k])

    def grad(chunk, saved, upstream, lane0, half):
        rows = upstream.shape[1] // 2
        r = rows // 8
        res = lax.dot_general(
            upstream[:, half * rows : (half + 1) * rows],
            saved[:, lane0 : lane0 + 512],
            (((0,), (0,)), ((), ())),
            preferred_element_type=F32,
        ).astype(BF)
        for xl in range(2):
            for yy in range(4):
                for zz in range(4):
                    at = {"x": half * 2 + xl, "y": yy, "z": zz}
                    r0 = (xl * 4 + yy) * r
                    for t, nr in enumerate(STREAMS[chunk]):
                        d1, d2, d3 = (at[d] for d in ORDER[t])
                        v[f"a1{chunk}{t}"][d1, pl.ds((d2 * 4 + d3) * nr, nr), :] = res[
                            r0 : r0 + nr, zz * 128 : zz * 128 + 128
                        ]
                        r0 += nr

    rsem = {}

    def rs_start(chunk, phase):
        for t in range(3):
            a, b = v[f"a{phase}{chunk}{t}"], v[f"r{phase}{chunk}{t}"]
            d = ORDER[t][phase - 1]
            ss, rs = sems.new(), sems.new()
            for k in (2, 1, 3):
                send(a.at[off(d, k)], b.at[k - 1], ss, rs, along(d, k))
            sent.append((b, ss))
            rsem[phase, chunk, t] = rs

    def rs_sum(chunk, phase, t):
        a, b = v[f"a{phase}{chunk}{t}"], v[f"r{phase}{chunk}{t}"]
        wait(b, rsem[phase, chunk, t])
        own = me[ORDER[t][phase - 1]]
        return (
            a[own].astype(F32) + b[0].astype(F32) + b[1].astype(F32) + b[2].astype(F32)
        ).astype(BF)

    def rs_next(chunk, phase):
        for t, nr in enumerate(STREAMS[chunk]):
            total = rs_sum(chunk, phase, t)
            dst = v[f"a{phase + 1}{chunk}{t}"]
            dst[...] = total.reshape(dst.shape)
        rs_start(chunk, phase + 1)

    gsem = {}

    def rs_end(chunk, g):
        r0 = 0
        for t, nr in enumerate(STREAMS[chunk]):
            g[z, pl.ds(r0, nr), :] = rs_sum(chunk, 3, t)
            r0 += nr
        ss, rs = sems.new(), sems.new()
        for k in (2, 1, 3):
            send(g.at[z], g.at[z], ss, rs, along("z", k))
        sent.append((g.at[pl.ds(0, 3)], ss))
        gsem[chunk] = rs

    def square_rows(total):
        hi = total.astype(BF).astype(F32)
        mid = (total - hi).astype(BF).astype(F32)
        low = total - hi - mid
        lane = lax.broadcasted_iota(jnp.int32, (16, 128), 1)
        row = lax.broadcasted_iota(jnp.int32, (16, 128), 0)
        out = jnp.where(lane == 0, hi, jnp.where(lane == 1, mid, jnp.where(lane == 2, low, 0.0)))
        return jnp.where(row == 0, out, 0.0).astype(BF)

    def total_of(a):
        return jnp.sum(jnp.sum(a, axis=1, keepdims=True), axis=0, keepdims=True)

    psem = {}

    def plane_send(k, src_of, dst):
        ss, rs = sems.new(), sems.new()
        for a in (2, 1, 3, 0):
            for b in (2, 1, 3, 0):
                if a or b:
                    send(src_of(off("x", a)), dst.at[x * 4 + y], ss, rs, dev(dx=a, dy=b))
        sent.append((dst.at[pl.ds(0, 15)], ss))
        psem[k] = rs

    def left_q():
        wait(v["gq"].at[pl.ds(0, 3)], gsem["q"])
        left_done("lq", 16)
        g = jnp.concatenate([v["gq"][k] for k in range(4)], axis=1)
        prod = lax.dot_general(
            g, v["lq"][...].reshape(128, 512), (((1,), (1,)), ((), ())), preferred_element_type=F32
        )
        gf = g.astype(F32)
        v["psq"][pl.ds(0, 48), :] = prod.astype(BF)
        v["psq"][pl.ds(48, 16), :] = square_rows(total_of(gf * gf))
        v["pq"][x * 4 + y] = v["psq"][...]
        plane_send("q", lambda k: v["psq"], v["pq"])

    def left_o():
        for ch in range(2):
            wait(v["go"].at[ch, pl.ds(0, 3)], gsem["ab"[ch]])
        left_done("lo", 32)
        g = jnp.concatenate([v["go"][h, k] for k in range(4) for h in range(2)], axis=1)
        prod = lax.dot_general(
            v["lo"][...].reshape(256, 1024),
            g,
            (((1,), (1,)), ((), ())),
            preferred_element_type=F32,
        )
        gf = g.astype(F32)
        sq = square_rows(total_of(gf * gf))
        for k in range(4):
            both = jnp.concatenate(
                [prod[k * 64 : k * 64 + 32], prod[k * 64 + 32 : k * 64 + 64]], axis=1
            )
            v["pso"][k, pl.ds(0, 32), :] = both.astype(BF)
            v["pso"][k, pl.ds(32, 16), :] = sq
        v["po"][x * 4 + y] = v["pso"][x]
        plane_send("o", lambda k: v["pso"].at[k], v["po"])

    csem = {}

    def core_send(k, direction, gsq):
        sq = direction * direction
        n = sq.shape[0] // 8
        rows = sum(sq[j * 8 : j * 8 + 8] for j in range(n))
        tile = sum(rows[:, j * 128 : j * 128 + 128] for j in range(sq.shape[1] // 128))
        v["cs" + k][pl.ds(0, 8), :] = tile
        v["cs" + k][pl.ds(8, 8), :] = jnp.broadcast_to(gsq, (8, 128))
        ss, rs = sems.new(), sems.new()
        send(v["cs" + k], v["cr" + k], ss, rs, dev(dc=1))
        sent.append((v["cr" + k], ss))
        csem[k] = rs

    def right_q():
        wait(v["pq"].at[pl.ds(0, 15)], psem["q"])
        ld["rq"].wait()
        for n in range(2):
            left = v["pq"][pl.ds(8 * n, 8), pl.ds(0, 48), :].reshape(384, 128)
            v["dq"][:, n * 384 : n * 384 + 384] = lax.dot_general(
                left, v["rq"][n], (((0,), (0,)), ((), ())), preferred_element_type=F32
            )
        gsq = total_of(sum(v["pq"][p, pl.ds(48, 16), :].astype(F32) for p in range(16)))
        core_send("q", v["dq"][pl.ds(x * 32, 32), :], gsq)

    def right_o():
        wait(v["po"].at[pl.ds(0, 15)], psem["o"])
        ld["ro"].wait()
        lane = lax.broadcasted_iota(jnp.int32, (32, 128), 1)
        top, low = [], []
        for j in range(8):
            p0 = v["po"][2 * j, pl.ds(0, 32), :].astype(F32)
            p1 = v["po"][2 * j + 1, pl.ds(0, 32), :].astype(F32)
            top.append(jnp.where(lane < 64, p0, pltpu.roll(p1, 64, 1)))
            low.append(jnp.where(lane < 64, pltpu.roll(p0, 64, 1), p1))
        for n in range(2):
            left = jnp.concatenate(
                [
                    jnp.concatenate(top[4 * n : 4 * n + 4], axis=1),
                    jnp.concatenate(low[4 * n : 4 * n + 4], axis=1),
                ],
                axis=0,
            ).astype(BF)
            v["do"][:, n * 512 : n * 512 + 512] = jnp.dot(
                left, v["ro"][n], preferred_element_type=F32
            )
        gsq = total_of(sum(v["po"][p, pl.ds(32, 16), :].astype(F32) for p in range(16)))
        core_send("o", v["do"][...], gsq)

    ssem = {}

    def sums_send(k):
        wait(v["cr" + k], csem[k])
        v[f"ps{k}2"][...] = v["cs" + k][pl.ds(0, 8), :] + v["cr" + k][pl.ds(0, 8), :]
        v[f"pr{k}2"][fs] = v[f"ps{k}2"][...]
        ss, rs = sems.new(), sems.new()
        for a in (2, 1, 3, 0):
            for b in (2, 1, 3, 0):
                if a or b:
                    send(v[f"ps{k}2"], v[f"pr{k}2"].at[fs], ss, rs, dev(dz=a, dx=b))
        sent.append((v[f"pr{k}2"].at[pl.ds(0, 15)], ss))
        ssem[k] = rs

    outs = []

    def finish(k, direction):
        wait(v[f"pr{k}2"].at[pl.ds(0, 15)], ssem[k])
        dsq = total_of(sum(v[f"pr{k}2"][p] for p in range(16)))
        gsq = v["cs" + k][pl.ds(8, 1), pl.ds(0, 1)] + v["cr" + k][pl.ds(8, 1), pl.ds(0, 1)]
        scale = jnp.sqrt(gsq / (dsq + 1e-6))
        ld["w" + k].wait()
        ld["m" + k].wait()
        moment = 0.8 * v["m" + k][...] + scale * direction
        weight = 0.998 * v["w" + k][...] - 0.02 * moment
        v["c" + k][z, x] = weight.astype(BF)
        return moment, weight

    def keep(k, moment, weight, o_m, o_w):
        v["m" + k][...] = moment
        v["w" + k][...] = weight
        outs.append(local(v["m" + k], o_m))
        outs.append(local(v["w" + k], o_w))

    class Gather:
        def __init__(self, k, n1, n2, n3):
            self.buf = v["c" + k]
            self.lanes = [pl.ds(0, n1 * 128), pl.ds(n1 * 128, n2 * 128)]
            if n3:
                self.lanes.append(pl.ds(pl.multiple_of((n1 + n2 + y) * 128, 128), 128))
            self.s = {}

        def block(self, t, dz=0, dx=0):
            return self.buf.at[off("z", dz), off("x", dx), :, self.lanes[t]]

        def push(self, t, key, blocks, d):
            ss, rs = sems.new(), sems.new()
            for b in blocks:
                for k in (2, 1, 3):
                    send(self.block(t, *b), self.block(t, *b), ss, rs, along(d, k))
            n = 3 * len(blocks)
            size = self.size(t)
            ref = (
                self.buf.at[0, pl.ds(0, 3), :, size]
                if n == 3
                else self.buf.at[pl.ds(0, 3), pl.ds(0, 3), :, size]
            )
            sent.append((ref, ss))
            self.s[t, key] = (ref, rs)

        def size(self, t):
            return pl.ds(0, 128) if t == 2 else self.lanes[t]

        def ready(self, t, key):
            wait(*self.s[t, key])

        def start(self):
            self.push(0, "x", [(0, 0)], "x")
            self.push(1, "z", [(0, 0)], "z")
            if len(self.lanes) > 2:
                self.push(2, "x", [(0, 0)], "x")
                self.push(2, "z0", [(0, 0)], "z")
            self.push(0, "z0", [(0, 0)], "z")
            self.push(1, "x0", [(0, 0)], "x")

        def second(self):
            if len(self.lanes) > 2:
                self.ready(2, "x")
                near = [(0, 2), (0, 1), (0, 3)]
                self.push(2, "z1", near, "z")
                self.push(2, "y1", near, "y")
            self.ready(0, "x")
            self.push(0, "z1", [(0, 2), (0, 1), (0, 3)], "z")
            self.ready(1, "z")
            self.push(1, "x1", [(2, 0), (1, 0), (3, 0)], "x")

        def third(self):
            if len(self.lanes) > 2:
                self.ready(2, "z0")
                self.push(2, "y2", [(2, 0), (1, 0), (3, 0)], "y")
                self.ready(2, "z1")
                for k in (1, 2, 3):
                    self.push(2, f"y3{k}", [(2, k), (1, k), (3, k)], "y")

        def end(self):
            for t, key in list(self.s):
                if (t, key) in ((0, "x"), (1, "z"), (2, "x"), (2, "z0"), (2, "z1")):
                    continue
                self.ready(t, key)

    ld["uq"].wait()
    ld["sq"].wait()
    grad("q", v["sq"], v["uq"], 0, 0)
    grad("q", v["sq"], v["uq"], 0, 1)
    rs_start("q", 1)
    for k in range(4):
        ld[f"so0{k}"].wait()
    ld["uo"].wait()
    grad("a", v["so"], v["uo"], 0, 0)
    left_forward("lo", 32)
    left_forward("lq", 16)
    grad("a", v["so"], v["uo"], 0, 1)
    rs_start("a", 1)
    for k in range(4):
        ld[f"so1{k}"].wait()
    rs_next("q", 1)
    grad("b", v["so"], v["uo"], 512, 0)
    rs_next("q", 2)
    grad("b", v["so"], v["uo"], 512, 1)
    rs_start("b", 1)
    rs_end("q", v["gq"])
    rs_next("a", 1)
    left_q()
    rs_next("a", 2)
    rs_next("b", 1)
    rs_end("a", v["go"].at[0])
    right_q()
    rs_next("b", 2)
    sums_send("q")
    rs_end("b", v["go"].at[1])
    mq, wq = finish("q", v["dq"][pl.ds(x * 32, 32), :])
    gat_q = Gather("q", 3, 3, 0)
    left_o()
    gat_q.start()
    keep("q", mq, wq, o_mq, o_wq)
    right_o()
    gat_q.second()
    sums_send("o")
    gat_q.end()
    outs.append(local(v["cq"], o_cq))
    mo, wo = finish("o", v["do"][...])
    gat_o = Gather("o", 2, 2, 4)
    gat_o.start()
    keep("o", mo, wo, o_mo, o_wo)
    gat_o.second()
    gat_o.third()
    gat_o.end()
    outs.append(local(v["co"], o_co))
    for ref, ss in sent:
        wait(ref, ss)
    for cp in outs:
        cp.wait()
    assert sems.n <= N_SEMS, sems.n


def local_fn(*args):
    shapes = [
        ((32, 768), F32),
        ((32, 768), F32),
        ((4, 4, 32, 768), BF),
        ((64, 1024), F32),
        ((64, 1024), F32),
        ((4, 4, 64, 1024), BF),
    ]
    out = pl.pallas_call(
        kernel,
        name="update",
        out_shape=[jax.ShapeDtypeStruct(s, d) for s, d in shapes],
        in_specs=[HBM] * 12,
        out_specs=[HBM] * 6,
        scratch_shapes=[pltpu.VMEM(s, d) for s, d in SCRATCH.values()]
        + [pltpu.SemaphoreType.DMA((N_SEMS,))],
        compiler_params=pltpu.CompilerParams(
            collective_id=0, has_side_effects=True, vmem_limit_bytes=60 * 1024 * 1024
        ),
    )(*args)
    wq, mq, cq, wo, mo, co = out
    return wq, mq, cq.reshape(512, 768), wo, mo, co.reshape(1024, 1024)


def solution(mesh):
    return jax.shard_map(
        local_fn,
        mesh=mesh,
        in_specs=(
            P(("fs", "rep"), None),
            P(("fs", "rep"), "tp"),
            P("fs", "tp"),
            P("fs", "tp"),
            P("fs", None),
            P("tp", None, None),
            P(("fs", "rep"), None),
            P(("fs", "rep"), "tp"),
            P("fs", "tp"),
            P("fs", "tp"),
            P("fs", None),
            P("tp", None, None),
        ),
        out_specs=(
            P("fs", "tp"),
            P("fs", "tp"),
            P(None, "tp"),
            P("fs", "tp"),
            P("fs", "tp"),
            P(None, "tp"),
        ),
        check_vma=False,
    )
```
